256 devices in a mesh: kv: 32 (over z, x), tp: 8 (over y, core).
Axes of the slice: x: 4, y: 4, z: 8, core: 2. Of those that a mesh axis runs over, the one named last changes fastest.
Arguments:
- tokens: bfloat16 [384, 2048], P('tp', 'kv'), may hold values from -10.5 to 10.5
- norm_gain: float32 [2048], P('kv'), may hold values from 0.1 to 1.9
- w_query: bfloat16 [2048, 2048], P('kv', 'tp'), may hold values from -0.125 to 0.125
- w_forget: bfloat16 [2048, 2048], P('kv', 'tp'), may hold values from -0.125 to 0.125
- w_input: bfloat16 [2048, 2048], P('kv', 'tp'), may hold values from -0.125 to 0.125
- w_gate: bfloat16 [2048, 2048], P('kv', 'tp'), may hold values from -0.125 to 0.125
- lower_bound: float32 [2048], P('tp'), may hold values from 0 to 0.9
- head_gain: float32 [16, 128], P('tp'), may hold values from 0.1 to 1.9
- recur_state: float32 [384, 16, 128, 128], P('kv', 'tp'), may hold values from -3 to 3
- w_out: bfloat16 [2048, 2048], P('tp', 'kv'), may hold values from -0.125 to 0.125
- mixer_gain: float32 [2048], P('kv'), may hold values from 0.1 to 1.9
- w_up: bfloat16 [2048, 8192], P('kv', 'tp'), may hold values from -0.125 to 0.125
- w_down: bfloat16 [8192, 2048], P('tp', 'kv'), may hold values from -0.0625 to 0.0625
Outputs:
- next_tokens: bfloat16 [384, 2048], P('tp', 'kv')
- next_state: float32 [384, 16, 128, 128], P('kv', 'tp')
The draws below stay inside these ranges and needn't reach their ends.
All inputs are finite; a program needn't handle non-finite values.
Results may differ from the reference program's by a relative error of at most 0.03.
Values may be sent and summed in bfloat16 or wider, within the bound.
No kernel may reach another device: no remote copies, remote signals or barrier semaphores. Data moves between devices by JAX's collectives and lax.ppermute only.
A program may use at most 64 MiB of HBM per device.

```python
import jax
import jax.numpy as jnp
from jax import lax

D = 2048
HEADS = 16
KEY = 128
VAL = 128
FF = 8192
SEQS = 384
N_TP = 8


def draw_tokens(key, part):
    first_key = jax.random.fold_in(key, 11)
    column = jnp.arange(D, dtype=jnp.float32) / D - 0.5
    base_draw = jnp.clip(jax.random.normal(first_key, (SEQS, D), jnp.float32), -6.0, 6.0)
    values = base_draw * jnp.exp(jnp.log(3.0) * column)[None, :]
    return values.astype(jnp.bfloat16)


def block_scale(own_key, shape, pieces, least, high):
    factor_of, own = 1.0, jax.random.fold_in(own_key, 6)
    for axis_at, parts in pieces:
        heights = jnp.exp(jax.random.uniform(jax.random.fold_in(own, axis_at), (parts,), jnp.float32, least / len(pieces), high / len(pieces)))
        factor_of = factor_of * jnp.repeat(heights, shape[axis_at] // parts).reshape([-1 if axis == axis_at else 1 for axis in range(len(shape))])
    return factor_of


def noise(key, dims, width, most, split=(), held_as=jnp.bfloat16):
    drawn = width * jax.random.normal(key, dims, jnp.float32)
    if split:
        drawn = drawn * block_scale(key, dims, split, -0.22, 0.18)
    return jnp.clip(drawn, -most, most).astype(held_as)


def setup_inputs(seed: int = 0) -> dict:
    key_list = jax.random.split(jax.random.key(seed), 14)
    return {
        "tokens": draw_tokens(jax.random.fold_in(key_list[13], 71), 0),
        "norm_gain": jnp.clip(1.0 + 0.18 * jax.random.normal(key_list[1], (D,), jnp.float32), 0.1, 1.9),
        "w_query": noise(key_list[2], (D, HEADS * KEY), D ** -0.5, 0.125, ((0, 32), (1, 8))),
        "w_forget": noise(key_list[3], (D, HEADS * KEY), D ** -0.5, 0.125, ((0, 32), (1, 8))),
        "w_input": noise(key_list[4], (D, HEADS * VAL), D ** -0.5, 0.125, ((0, 32), (1, 8))),
        "w_gate": noise(key_list[5], (D, HEADS * VAL), D ** -0.5, 0.125, ((0, 32), (1, 8))),
        "lower_bound": jnp.clip(0.9 * jax.random.uniform(key_list[6], (HEADS * KEY,), jnp.float32) ** block_scale(key_list[6], (HEADS * KEY,), ((0, 8),), -0.2, 0.2), 0.0, 0.9),
        "head_gain": jnp.clip(1.0 + 0.18 * jax.random.normal(key_list[7], (HEADS, VAL), jnp.float32), 0.1, 1.9),
        "recur_state": noise(key_list[8], (SEQS, HEADS, KEY, VAL), 0.5, 3.0, ((0, 32), (1, 8)), jnp.float32),
        "w_out": noise(key_list[9], (HEADS * VAL, D), (HEADS * VAL) ** -0.5, 0.125, ((0, 8), (1, 32))),
        "mixer_gain": jnp.clip(1.0 + 0.18 * jax.random.normal(key_list[10], (D,), jnp.float32), 0.1, 1.9),
        "w_up": noise(key_list[11], (D, FF), D ** -0.5, 0.125, ((0, 32), (1, 8))),
        "w_down": noise(key_list[12], (FF, D), FF ** -0.5, 0.0625, ((0, 8), (1, 32))),
    }


NORM_EPS = 1e-05

def project(row_block, norm_scale, weight):
    tokens_f = row_block.astype(jnp.float32)
    row_scale = lax.rsqrt(lax.optimization_barrier(jnp.mean(tokens_f * tokens_f, axis=1)) + NORM_EPS)
    normed = (tokens_f * norm_scale).astype(jnp.bfloat16)
    return jnp.dot(normed, weight, preferred_element_type=jnp.float32) * row_scale[:, None]

def grouped(values_bf, weight):
    count = values_bf.shape[0]
    grouped_vals = values_bf.reshape(count, N_TP, -1).astype(jnp.float32)
    grouped_mats = weight.reshape(N_TP, -1, weight.shape[1]).astype(jnp.float32)
    partials = jnp.einsum('rgc,gcd->grd', grouped_vals, grouped_mats)
    return lax.optimization_barrier(jnp.sum(partials.astype(jnp.bfloat16).astype(jnp.float32), axis=0))

def reference(tokens, norm_gain, w_query, w_forget, w_input, w_gate, lower_bound, head_gain, recur_state, w_out, mixer_gain, w_up, w_down):
    count = tokens.shape[0]
    queries = project(tokens, norm_gain, w_query).reshape(count, HEADS, KEY)
    forget_raw = project(tokens, norm_gain, w_forget).reshape(count, HEADS, KEY)
    values_in = project(tokens, norm_gain, w_input).reshape(count, HEADS, VAL)
    gate_raw = project(tokens, norm_gain, w_gate)
    bound = lower_bound.reshape(HEADS, KEY)
    forget = bound + (1.0 - bound) * jax.nn.sigmoid(forget_raw)
    next_state = forget[..., None] * recur_state + (1.0 - forget)[..., None] * values_in[:, :, None, :]
    read_out = jnp.einsum('rhk,rhkv->rhv', queries, next_state, precision=lax.Precision.HIGHEST)
    read_out = read_out * lax.rsqrt(lax.optimization_barrier(jnp.mean(read_out * read_out, axis=2, keepdims=True)) + NORM_EPS) * head_gain
    mixture = (read_out.reshape(count, HEADS * VAL) * jax.nn.silu(gate_raw)).astype(jnp.bfloat16)
    mixed_rows = (tokens.astype(jnp.float32) + grouped(mixture, w_out)).astype(jnp.bfloat16)
    hidden_pre = project(mixed_rows, mixer_gain, w_up)
    hidden = jnp.square(jax.nn.relu(hidden_pre)).astype(jnp.bfloat16)
    next_tokens = (mixed_rows.astype(jnp.float32) + grouped(hidden, w_down)).astype(jnp.bfloat16)
    return (next_tokens, next_state)
```

```python
import jax
import jax.numpy as jnp
from jax import lax
from jax.experimental import pallas as pl
from jax.experimental.pallas import tpu as pltpu
from jax.sharding import PartitionSpec as P

NORM_EPS = 1e-05
AXES = ("kv", "tp")
NZ, NX, NY, NC = 8, 4, 4, 2
BF, F32 = jnp.bfloat16, jnp.float32


def flat(z, x, y, c):
    return ((z * NX + x) * NY + y) * NC + c


def send(value, to):
    pairs = []
    for z in range(NZ):
        for x in range(NX):
            for y in range(NY):
                for c in range(NC):
                    pairs.append((flat(z, x, y, c), flat(*to(z, x, y, c))))
    return lax.ppermute(value, AXES, pairs)


def to_z(value, k):
    return send(value, lambda z, x, y, c: ((z + k) % NZ, x, y, c))


def to_x(value, k):
    return send(value, lambda z, x, y, c: (z, (x + k) % NX, y, c))


def to_y(value, k):
    return send(value, lambda z, x, y, c: (z, x, (y + k) % NY, c))


def to_core(value):
    return send(value, lambda z, x, y, c: (z, x, y, 1 - c))


def swap_rows(value):
    return send(value, lambda z, x, y, c: (NC * y + c, x, z // NC, z % NC))


def ring(shard, halves):
    got = [shard] + [None] * (NZ - 1)
    up, down = shard, shard
    for k in range(1, NZ // 2):
        up, down = to_z(up, 1), to_z(down, -1)
        got[NZ - k], got[k] = up, down
    first, second = halves
    a = to_z(up[first], 1)
    b = to_z(down[second], -1)
    got[NZ // 2] = (a, b)
    return got


def nt(a, b):
    return lax.dot_general(a, b, (((1,), (1,)), ((), ())), preferred_element_type=F32)


def nn(a, b):
    return jnp.dot(a, b, preferred_element_type=F32)


def lane_squares(v):
    s = v * v
    return (s[:, 0:128] + s[:, 128:256]) + (s[:, 256:384] + s[:, 384:512])


def call(kernel, outs, *args, scratch=()):
    in_specs = [
        pl.BlockSpec(memory_space=pltpu.SMEM if a.dtype == jnp.int32 else pltpu.VMEM) for a in args
    ]
    return pl.pallas_call(
        kernel,
        out_shape=outs,
        in_specs=in_specs,
        out_specs=jax.tree.map(lambda _: pl.BlockSpec(memory_space=pltpu.VMEM), outs),
        scratch_shapes=scratch,
    )(*args)


def project_kernel(tok_at, row_at, tok, w0, w1, w2, w3, w4a, w4b, w5, w6, w7, *rest):
    outs, acc = rest[:NX], rest[NX]
    xs = [tok[tok_at[k]] for k in range(NZ)]
    x_lo = jnp.concatenate(xs[:4], axis=1)
    x_hi = jnp.concatenate(xs[4:], axis=1)
    w_lo = jnp.concatenate([w[:, :1024] for w in (w0, w1, w2, w3)], axis=0)
    w_hi = jnp.concatenate([w[:, :1024] for w in (w4a, w4b, w5, w6, w7)], axis=0)
    main = nn(x_lo, w_lo) + nn(x_hi, w_hi)
    squares = lane_squares(jnp.concatenate([x_lo, x_hi], axis=1).astype(F32))
    for i in range(NX):
        acc[i, :, :1024] = main[12 * i : 12 * i + 12]
        acc[i, :, 1024:] = squares[12 * i : 12 * i + 12]
    for k in range(NX):
        outs[k][...] = acc[row_at[k]].astype(BF)


def attend_kernel(row_at, m0, m1, m2, m3, w0, w1, w2, w3, w4a, w4b, w5, w6, w7, out, acc):
    for k, m in enumerate((m0, m1, m2, m3)):
        acc[row_at[k]] = m[...].astype(F32)
    mix = jnp.concatenate([acc[i] for i in range(NX)], axis=0).astype(BF)
    w = jnp.concatenate([w[:, 1024:] for w in (w0, w1, w2, w3, w4a, w4b, w5, w6, w7)], axis=0)
    out[...] = nt(mix, w).astype(BF)


def up_kernel(tok_at, s0, s1, s2, s3, tok, w0, w1, w2, w3, w4, w5, w6, w7, mixed, msg):
    total = (s0[...].astype(F32) + s1[...].astype(F32)) + (s2[...].astype(F32) + s3[...].astype(F32))
    x = jnp.concatenate([tok[tok_at[k]] for k in range(NZ)], axis=1).astype(F32)
    rows = (x + total).astype(BF)
    mixed[...] = rows
    w = jnp.concatenate([w[:64, :] for w in (w0, w1, w2, w3, w4, w5, w6, w7)], axis=0)
    msg[:, :1024] = nn(rows, w).astype(BF)
    msg[:, 1024:] = lane_squares(rows.astype(F32)).astype(BF)


def down_kernel(put_at, h0, h1, h2, h3, w0, w1, w2, w3, w4, w5, w6, w7, out):
    total = (h0[...].astype(F32) + h1[...].astype(F32)) + (h2[...].astype(F32) + h3[...].astype(F32))
    scale = lax.rsqrt(jnp.sum(total[:, 1024:], axis=1, keepdims=True) / 2048 + NORM_EPS)
    hidden = jnp.square(jnp.maximum(total[:, :1024] * scale, 0.0)).astype(BF)
    ws = [w0[64:, :], w1[64:, :], w2[64:, :], w3[64:, :], w4[...], w5[64:, :], w6[64:, :], w7[64:, :]]
    part = nt(hidden, jnp.concatenate(ws, axis=0)).astype(BF)
    for k in range(NZ):
        out[put_at[k]] = part[:, 64 * k : 64 * (k + 1)]


def body(
    tokens, norm_gain, w_query, w_forget, w_input, w_gate, lower_bound, head_gain, recur_state,
    w_out, mixer_gain, w_up, w_down,
):
    kv, tp = lax.axis_index("kv"), lax.axis_index("tp")
    z, x, y, c = kv // NX, kv % NX, tp // NC, tp % NC
    kz = (z + jnp.arange(NZ)) % NZ
    tok_at = ((kz // NC - y) % NY * NC + (kz + c) % NC).astype(jnp.int32)
    put_at = ((kz + c) % NC * NY + (kz // NC - y) % NY).astype(jnp.int32)
    row_at = ((x + jnp.arange(NX)) % NX).astype(jnp.int32)

    w_in = jnp.concatenate([w_query, w_forget, w_input, w_gate], axis=1).astype(F32)
    early = jnp.concatenate([(w_in * norm_gain[:, None]).astype(BF), w_out.T], axis=1)
    late = jnp.concatenate([(w_up.astype(F32) * mixer_gain[:, None]).astype(BF), w_down.T], axis=0)

    mine = swap_rows(tokens)
    pair = jnp.stack([mine, to_core(mine)])
    tok = jnp.concatenate([pair] + [to_y(pair, -j) for j in range(1, NY)], axis=0)

    e = ring(early, (slice(0, 32), slice(32, 64)))
    ea, eb = e[4]
    ew = (*e[:4], ea, eb, *e[5:])
    parts = call(
        project_kernel,
        [jax.ShapeDtypeStruct((12, 1152), BF)] * NX,
        tok_at, row_at, tok, *ew,
        scratch=[pltpu.VMEM((NX, 12, 1152), F32)],
    )
    total = parts[0].astype(F32)
    for k in range(1, NX):
        total = total + to_x(parts[k], k).astype(F32)
    scale = lax.rsqrt(jnp.sum(total[:, 1024:], axis=1) / 2048 + NORM_EPS)
    projected = total[:, :1024] * scale[:, None]

    queries = projected[:, :256].reshape(12, 2, 128)
    forget_raw = projected[:, 256:512].reshape(12, 2, 128)
    values_in = projected[:, 512:768].reshape(12, 2, 128)
    gate_raw = projected[:, 768:]
    bound = lower_bound.reshape(2, 128)
    forget = bound + (1.0 - bound) * jax.nn.sigmoid(forget_raw)
    next_state = (
        forget[..., None] * recur_state + (1.0 - forget)[..., None] * values_in[:, :, None, :]
    )
    read_out = jnp.einsum("rhk,rhkv->rhv", queries, next_state, precision=lax.Precision.HIGHEST)
    read_out = (
        read_out
        * lax.rsqrt(jnp.mean(read_out * read_out, axis=2, keepdims=True) + NORM_EPS)
        * head_gain
    )
    mixture = (read_out.reshape(12, 256) * jax.nn.silu(gate_raw)).astype(BF)

    mixes = [mixture] + [to_x(mixture, -k) for k in range(1, NX)]
    attn = call(
        attend_kernel,
        jax.ShapeDtypeStruct((48, 512), BF),
        row_at, *mixes, *ew,
        scratch=[pltpu.VMEM((NX, 12, 256), F32)],
    )
    duo = (attn.astype(F32) + to_core(attn).astype(F32)).astype(BF)
    sums = [duo] + [to_y(duo, k) for k in range(1, NY)]

    f = ring(late, (slice(0, 64), slice(64, 128)))
    up4, down4 = f[4]
    mixed, msg = call(
        up_kernel,
        [jax.ShapeDtypeStruct((48, 512), BF), jax.ShapeDtypeStruct((48, 1152), BF)],
        tok_at, *sums, tok, *f[:4], up4, *f[5:],
    )
    msgs = [msg] + [to_x(msg, k) for k in range(1, NX)]
    blocks = call(
        down_kernel,
        jax.ShapeDtypeStruct((NZ, 48, 64), BF),
        put_at, *msgs, *f[:4], down4, *f[5:],
    )
    kept = (blocks[:NY].astype(F32) + to_core(blocks[NY:]).astype(F32)).astype(BF)
    down_out = kept[0].astype(F32)
    for k in range(1, NY):
        down_out = down_out + to_y(kept[k], k).astype(F32)
    own = lax.dynamic_slice_in_dim(mixed, (tp - z) % NZ * 64, 64, 1)
    next_tokens = swap_rows((own.astype(F32) + down_out).astype(BF))
    return (next_tokens, next_state)


def solution(mesh):
    in_specs = (
        P("tp", "kv"),
        P("kv"),
        P("kv", "tp"),
        P("kv", "tp"),
        P("kv", "tp"),
        P("kv", "tp"),
        P("tp"),
        P("tp", None),
        P("kv", "tp", None, None),
        P("tp", "kv"),
        P("kv"),
        P("kv", "tp"),
        P("tp", "kv"),
    )
    out_specs = (P("tp", "kv"), P("kv", "tp", None, None))
    return jax.shard_map(body, mesh=mesh, in_specs=in_specs, out_specs=out_specs, check_vma=False)
```

```python
import jax
import jax.numpy as jnp
from jax import lax
from jax.experimental import pallas as pl
from jax.experimental.pallas import tpu as pltpu
from jax.sharding import Mesh, PartitionSpec as P

NORM_EPS = 1e-05
NZ, NX, NY, NC = 8, 4, 4, 2
NT = NY * NC
AXES = ("z", "x", "y", "core")
TP = ("y", "core")
XTP = ("x", "y", "core")
BF, F32 = jnp.bfloat16, jnp.float32


def flat(z, x, y, c):
    return ((z * NX + x) * NY + y) * NC + c


def send(value, to):
    pairs = []
    for z in range(NZ):
        for x in range(NX):
            for y in range(NY):
                for c in range(NC):
                    pairs.append((flat(z, x, y, c), flat(*to(z, x, y, c))))
    return lax.ppermute(value, AXES, pairs)


def to_x(value, k):
    return send(value, lambda z, x, y, c: (z, (x + k) % NX, y, c))


def swap_rows(value):
    return send(value, lambda z, x, y, c: (NC * y + c, x, z // NC, z % NC))


def exchange(tiles, axis):
    return lax.all_to_all(tiles, axis, 0, 0, tiled=True)


def gathered(value, axis):
    size = lax.axis_size(axis)
    return exchange(jnp.broadcast_to(value[None], (size, *value.shape)), axis)


def after(value, *others):
    return lax.optimization_barrier((value, *others))[0]


def nt(a, b, precision=None):
    return lax.dot_general(
        a, b, (((1,), (1,)), ((), ())), preferred_element_type=F32, precision=precision
    )


def with_squares(main, rows):
    n = main.shape[0] // 16
    sums = nt(jnp.ones((8, rows.shape[1]), F32), rows * rows, lax.Precision.HIGHEST)[:1]
    if n * 16 < 128:
        sums = jnp.concatenate([sums, jnp.zeros((1, 128 - n * 16), F32)], axis=1)
    high = sums.astype(BF).astype(F32)
    low = sums - high
    row = lax.broadcasted_iota(jnp.int32, (n, 16, 128), 1)
    cube = main.reshape(n, 16, 1024)
    head = jnp.where(row == 12, high[None], jnp.where(row == 13, low[None], cube[:, :, :128]))
    return jnp.concatenate([head, cube[:, :, 128:]], axis=2).astype(BF)


def scaled(total, place):
    sums = total[12:13, :128] + total[13:14, :128]
    row = lax.broadcasted_iota(jnp.int32, (16, 128), 0)
    lane = lax.broadcasted_iota(jnp.int32, (16, 128), 1)
    mine = jnp.where((lane == row + 16 * place) & (row < 12), sums, 0.0)
    square = jnp.sum(mine, axis=1, keepdims=True)
    return total * lax.rsqrt(square / 2048 + NORM_EPS)


def call(kernel, outs, *args, scratch=()):
    in_specs = [
        pl.BlockSpec(memory_space=pltpu.SMEM if a.dtype == jnp.int32 else pltpu.VMEM) for a in args
    ]
    return pl.pallas_call(
        kernel,
        out_shape=outs,
        in_specs=in_specs,
        out_specs=jax.tree.map(lambda _: pl.BlockSpec(memory_space=pltpu.VMEM), outs),
        scratch_shapes=scratch,
    )(*args)


def shape(*dims, dtype=BF):
    return jax.ShapeDtypeStruct(dims, dtype)


def project_kernel(tok, w, out):
    x = jnp.concatenate([tok[i].reshape(128, 64) for i in range(NX)], axis=1)
    main = jnp.dot(x, w[...].reshape(256, 1024), preferred_element_type=F32)
    out[...] = with_squares(main, x.astype(F32))


def recur_kernel(place, msg, state, bound, gain, mixture, new):
    total = msg[0].astype(F32)
    for k in range(1, NZ):
        total = total + msg[k].astype(F32)
    total = scaled(total, place[0])
    reads = [[], []]
    for h in range(2):
        at = slice(128 * h, 128 * h + 128)
        low = bound[:, at]
        forget = low + (1.0 - low) * jax.nn.sigmoid(total[:, 256:512][:, at])
        f_t = forget.T
        q_t = total[:, :256][:, at].T
        v = total[:, 512:768][:, at]
        for r in range(12):
            row = v[r : r + 1]
            s = row + f_t[:, r : r + 1] * (state[r, h] - row)
            new[r, h] = s
            reads[h].append(jnp.sum(q_t[:, r : r + 1] * s, axis=0, keepdims=True))
    for h in range(2):
        at = slice(128 * h, 128 * h + 128)
        read = jnp.concatenate(reads[h] + [jnp.zeros((4, 128), F32)], axis=0)
        read = read * lax.rsqrt(jnp.mean(read * read, axis=1, keepdims=True) + NORM_EPS)
        mixture[:, at] = (read * gain[h : h + 1] * jax.nn.silu(total[:, 768:][:, at])).astype(BF)


def attend_kernel(row_at, m0, m1, m2, m3, w, tok, out, acc):
    for k, m in enumerate((m0, m1, m2, m3)):
        acc[row_at[k]] = m[...]
    part = nt(acc[...].reshape(64, 256), w[...].reshape(512, 256))
    part = jnp.concatenate([part[16 * i : 16 * i + 12] for i in range(NX)], axis=0)
    part = (part + tok[...].astype(F32)).astype(BF)
    for k in range(NT):
        out[k] = part


def up_kernel(row_at, parts, w, mixed, o0, o1, o2, o3, acc):
    total = parts[0].astype(F32)
    for k in range(1, NT):
        total = total + parts[k].astype(F32)
    rows = total.astype(BF)
    mixed[...] = rows
    wide = rows.astype(F32)
    pad = jnp.zeros((4, 512), F32)
    pieces = [p for i in range(NX) for p in (wide[12 * i : 12 * i + 12], pad)]
    wide = jnp.concatenate(pieces, axis=0)
    main = jnp.dot(wide.astype(BF), w[...].reshape(512, 1024), preferred_element_type=F32)
    acc[...] = with_squares(main, wide)
    for k, o in enumerate((o0, o1, o2, o3)):
        o[...] = acc[row_at[k]]


def hidden_kernel(place, m0, m1, m2, m3, out):
    total = (m0[...].astype(F32) + m1[...].astype(F32)) + (m2[...].astype(F32) + m3[...].astype(F32))
    row = lax.broadcasted_iota(jnp.int32, (16, 1024), 0)
    pre = jnp.where(row < 12, scaled(total, place[0]), 0.0)
    hidden = jnp.square(jnp.maximum(pre, 0.0)).astype(BF)
    for k in range(NZ):
        out[k] = hidden


def down_kernel(hidden, w, out):
    part = nt(hidden[...].reshape(128, 1024), w[...].reshape(256, 1024)).astype(BF)
    for i in range(NX):
        out[i] = part[:, 64 * i : 64 * i + 64].reshape(NZ, 16, 64)


def last_kernel(parts, mixed, out):
    for i in range(NX):
        total = parts[i, 0].astype(F32)
        for k in range(1, NT):
            total = total + parts[i, k].astype(F32)
        out[12 * i : 12 * i + 12, :] = total[:12] + mixed[12 * i : 12 * i + 12, :].astype(F32)


def body(
    tokens, norm_gain, w_query, w_forget, w_input, w_gate, lower_bound, head_gain, recur_state,
    w_out, mixer_gain, w_up, w_down,
):
    z, x = lax.axis_index("z"), lax.axis_index("x")
    t = lax.axis_index(TP)
    row_at = ((x + jnp.arange(NX)) % NX).astype(jnp.int32)
    z_at, x_at = z.reshape(1).astype(jnp.int32), x.reshape(1).astype(jnp.int32)

    cut = jnp.pad(tokens.reshape(NX, 1, 12, 64), ((0, 0), (0, 0), (0, 4), (0, 0)))
    cut = jnp.broadcast_to(cut, (NX, NT, 16, 64)).reshape(NX * NT, 16, 64)
    tok = exchange(cut, XTP).reshape(NX, NT, 16, 64)
    w_in = jnp.concatenate([w_query, w_forget, w_input, w_gate], axis=1).astype(F32)
    w_in = gathered((w_in * norm_gain[:, None]).astype(BF), "x")
    moved = swap_rows(tokens)
    w_out = gathered(w_out.T, "z")

    parts = call(project_kernel, shape(NZ, 16, 1024), tok, w_in)
    w_down = gathered(after(w_down.T, parts), "x")
    msg = exchange(parts, "z")
    w_up = (w_up.astype(F32) * mixer_gain[:, None]).astype(BF)
    w_up = gathered(after(w_up, msg), "z")
    mixture, next_state = call(
        recur_kernel,
        [shape(16, 256), shape(12, 2, 128, 128, dtype=F32)],
        z_at, msg, recur_state, lower_bound.reshape(1, 256), head_gain,
    )

    mixes = [mixture] + [to_x(mixture, -k) for k in range(1, NX)]
    block = lax.broadcasted_iota(jnp.int32, (48, 512), 1) // 64
    spread = jnp.where(block == t, jnp.tile(moved, (1, NZ)), jnp.zeros((), BF))
    attn = call(
        attend_kernel,
        shape(NT, 48, 512),
        row_at, *mixes, w_out, spread,
        scratch=[pltpu.VMEM((NX, 16, 256), BF)],
    )
    mixed, *outs = call(
        up_kernel,
        [shape(48, 512)] + [shape(16, 1024)] * NX,
        row_at, exchange(attn, TP), w_up,
        scratch=[pltpu.VMEM((NX, 16, 1024), BF)],
    )
    ups = [outs[0]] + [to_x(outs[k], k) for k in range(1, NX)]
    home = swap_rows(lax.dynamic_slice_in_dim(mixed, t * 64, 64, 1))
    hidden = exchange(call(hidden_kernel, shape(NZ, 16, 1024), x_at, *ups), "z")
    downs = call(down_kernel, shape(NX, NT, 16, 64), hidden, w_down)
    back = exchange(downs.reshape(NX * NT, 16, 64), XTP).reshape(NX, NT, 16, 64)
    last = call(last_kernel, shape(48, 64, dtype=F32), back, home)
    return (last.astype(BF), next_state)


def solution(mesh):
    devices = mesh.devices.reshape(NZ, NX, NY, NC)
    kv, tp = ("z", "x"), TP
    in_specs = (
        P(tp, kv),
        P(kv),
        P(kv, tp),
        P(kv, tp),
        P(kv, tp),
        P(kv, tp),
        P(tp),
        P(tp, None),
        P(kv, tp, None, None),
        P(tp, kv),
        P(kv),
        P(kv, tp),
        P(tp, kv),
    )
    out_specs = (P(tp, kv), P(kv, tp, None, None))
    return jax.shard_map(
        body, mesh=Mesh(devices, AXES), in_specs=in_specs, out_specs=out_specs, check_vma=False
    )
```

```python
import jax
import jax.numpy as jnp
from jax import lax
from jax.experimental import pallas as pl
from jax.experimental.pallas import tpu as pltpu
from jax.sharding import Mesh, PartitionSpec as P


NORM_EPS = 1e-05
NZ, NX, NY, NC = 8, 4, 4, 2
NT = NY * NC
AXES = ("z", "x", "y", "core")
TP = ("y", "core")
XTP = ("x", "y", "core")
BF, F32 = jnp.bfloat16, jnp.float32


def flat(z, x, y, c):
    return ((z * NX + x) * NY + y) * NC + c


def send(value, to):
    pairs = []
    for z in range(NZ):
        for x in range(NX):
            for y in range(NY):
                for c in range(NC):
                    pairs.append((flat(z, x, y, c), flat(*to(z, x, y, c))))
    return lax.ppermute(value, AXES, pairs)


def to_z(value, k):
    return send(value, lambda z, x, y, c: ((z + k) % NZ, x, y, c))


def to_x(value, k):
    return send(value, lambda z, x, y, c: (z, (x + k) % NX, y, c))


def to_y(value, k):
    return send(value, lambda z, x, y, c: (z, x, (y + k) % NY, c))


def to_core(value):
    return send(value, lambda z, x, y, c: (z, x, y, 1 - c))


def swap_rows(value):
    return send(value, lambda z, x, y, c: (NC * y + c, x, z // NC, z % NC))


def exchange(tiles, axis):
    return lax.all_to_all(tiles, axis, 0, 0, tiled=True)


def after(value, *others):
    return lax.optimization_barrier((value, *others))[0]


def nt(a, b, precision=None):
    return lax.dot_general(
        a, b, (((1,), (1,)), ((), ())), preferred_element_type=F32, precision=precision
    )


def nn(a, b):
    return jnp.dot(a, b, preferred_element_type=F32)


def with_squares(main, rows):
    n = main.shape[0] // 16
    sums = nt(jnp.ones((8, rows.shape[1]), F32), rows * rows, lax.Precision.HIGHEST)[:1]
    high = sums.astype(BF).astype(F32)
    low = sums - high
    row = lax.broadcasted_iota(jnp.int32, (n, 16, 128), 1)
    cube = main.reshape(n, 16, 1024)
    head = jnp.where(row == 12, high[None], jnp.where(row == 13, low[None], cube[:, :, :128]))
    return jnp.concatenate([head, cube[:, :, 128:]], axis=2).astype(BF)


def scaled(total, place):
    sums = total[12:13, :128] + total[13:14, :128]
    row = lax.broadcasted_iota(jnp.int32, (16, 128), 0)
    lane = lax.broadcasted_iota(jnp.int32, (16, 128), 1)
    mine = jnp.where((lane == row + 16 * place) & (row < 12), sums, 0.0)
    square = jnp.sum(mine, axis=1, keepdims=True)
    return total * lax.rsqrt(square / 2048 + NORM_EPS)


def lane_squares(v):
    s = v * v
    return (s[:, 0:128] + s[:, 128:256]) + (s[:, 256:384] + s[:, 384:512])


def call(kernel, outs, *args, scratch=()):
    in_specs = [
        pl.BlockSpec(memory_space=pltpu.SMEM if a.dtype == jnp.int32 else pltpu.VMEM) for a in args
    ]
    args = [
        a if a.dtype == jnp.int32 else pltpu.with_memory_space_constraint(a, pltpu.VMEM)
        for a in args
    ]
    return pl.pallas_call(
        kernel,
        out_shape=outs,
        in_specs=in_specs,
        out_specs=jax.tree.map(lambda _: pl.BlockSpec(memory_space=pltpu.VMEM), outs),
        scratch_shapes=scratch,
    )(*args)


def shape(*dims, dtype=BF):
    return jax.ShapeDtypeStruct(dims, dtype)


def local(*dims, dtype=BF):
    return pltpu.VMEM(dims, dtype)


def spread_kernel(tok, out):
    wide = tok[...].astype(F32)
    pad = jnp.zeros((4, 64), F32)
    for i in range(NX):
        rows = jnp.concatenate([wide[12 * i : 12 * i + 12], pad], axis=0)
        tile = jnp.concatenate([rows[:8], rows[8:]], axis=1).astype(BF)
        for k in range(NT):
            out[NT * i + k] = tile


def fold_kernel(wq, wf, wi, wg, gain, out):
    for k, w in enumerate((wq, wf, wi, wg)):
        out[:, 256 * k : 256 * k + 256] = (w[...].astype(F32) * gain[...]).astype(BF)


def project_kernel(x_at, tok, w0, w1, w2, w3, out, both):
    for i in range(NX):
        part = tok[NT * i : NT * i + NT]
        both[i] = jnp.concatenate([part[:, :, :64], part[:, :, 64:]], axis=1).reshape(128, 64)
    x = jnp.concatenate([both[x_at[k]] for k in range(NX)], axis=1)
    main = nn(x, jnp.concatenate([w[...] for w in (w0, w1, w2, w3)], axis=0))
    out[...] = with_squares(main, x.astype(F32))


def recur_kernel(place, msg, bound, gain, state_hbm, mixture, new_hbm, state, new, came, went):
    reading = [pltpu.make_async_copy(state_hbm.at[r], state.at[r], came.at[r]) for r in range(12)]
    writing = [pltpu.make_async_copy(new.at[r], new_hbm.at[r], went.at[r]) for r in range(12)]
    for copy in reading:
        copy.start()
    total = msg[0].astype(F32)
    for k in range(1, NZ):
        total = total + msg[k].astype(F32)
    total = scaled(total, place[0])
    reads = [[], []]
    low = bound[...]
    forget = low + (1.0 - low) * jax.nn.sigmoid(total[:, 256:512])
    f_t = [forget[:, :128].T, forget[:, 128:].T]
    q_t = [total[:, :128].T, total[:, 128:256].T]
    v = total[:, 512:768]
    for r in range(12):
        reading[r].wait()
        for h in range(2):
            row = v[r : r + 1, 128 * h : 128 * h + 128]
            s = row + f_t[h][:, r : r + 1] * (state[r, h] - row)
            new[r, h] = s
            reads[h].append(jnp.sum(q_t[h][:, r : r + 1] * s, axis=0, keepdims=True))
        writing[r].start()
    for h in range(2):
        at = slice(128 * h, 128 * h + 128)
        read = jnp.concatenate(reads[h] + [jnp.zeros((4, 128), F32)], axis=0)
        read = read * lax.rsqrt(jnp.mean(read * read, axis=1, keepdims=True) + NORM_EPS)
        mixture[:, at] = (read * gain[h : h + 1] * jax.nn.silu(total[:, 768:][:, at])).astype(BF)
    for copy in writing:
        copy.wait()


def attend_kernel(x_at, m0, m1, m2, m3, *rest):
    ws, (tok, out, acc) = rest[:NZ], rest[NZ:]
    for k, m in enumerate((m0, m1, m2, m3)):
        acc[x_at[k]] = m[...]
    ws = [w if w.shape[0] == 16 else w.at[128:144] for w in ws]
    w = jnp.concatenate([w[:, 256 * j : 256 * j + 256] for w in ws for j in range(4)], axis=0)
    part = nt(acc[...].reshape(64, 256), w)
    part = jnp.concatenate([part[16 * i : 16 * i + 12] for i in range(NX)], axis=0)
    out[...] = (part + tok[...].astype(F32)).astype(BF)


def pair_kernel(a, b, out):
    out[...] = (a[...].astype(F32) + b[...].astype(F32)).astype(BF)


def up_kernel(s0, s1, s2, s3, *rest):
    ws, (mixed, msg) = rest[:NZ], rest[NZ:]
    total = (s0[...].astype(F32) + s1[...].astype(F32)) + (s2[...].astype(F32) + s3[...].astype(F32))
    rows = total.astype(BF)
    mixed[...] = rows
    w = jnp.concatenate([w[:64, :] for w in ws], axis=0)
    msg[:, :1024] = nn(rows, w).astype(BF)
    msg[:, 1024:] = lane_squares(rows.astype(F32)).astype(BF)


def down_kernel(put_at, h0, h1, h2, h3, *rest):
    ws, (keep, give, acc) = rest[:NZ], rest[NZ:]
    total = (h0[...].astype(F32) + h1[...].astype(F32)) + (h2[...].astype(F32) + h3[...].astype(F32))
    scale = lax.rsqrt(jnp.sum(total[:, 1024:], axis=1, keepdims=True) / 2048 + NORM_EPS)
    hidden = jnp.square(jnp.maximum(total[:, :1024] * scale, 0.0)).astype(BF)
    part = nt(hidden, jnp.concatenate([w[...] if w.shape[0] == 64 else w[64:128, :] for w in ws], axis=0)).astype(BF)
    for k in range(NZ):
        acc[put_at[k]] = part[:, 64 * k : 64 * (k + 1)]
    keep[...] = acc[:NY]
    give[...] = acc[NY:]


def halve_kernel(kept, came, o0, o1, o2, o3):
    for k, o in enumerate((o0, o1, o2, o3)):
        o[...] = (kept[k].astype(F32) + came[k].astype(F32)).astype(BF)


def last_kernel(k_at, mixed, p0, p1, p2, p3, out, acc):
    for k in range(NZ):
        acc[k] = mixed[:, 64 * k : 64 * k + 64]
    total = (p0[...].astype(F32) + p1[...].astype(F32)) + (p2[...].astype(F32) + p3[...].astype(F32))
    out[...] = (acc[k_at[0]].astype(F32) + total).astype(BF)


def body(
    tokens, norm_gain, w_query, w_forget, w_input, w_gate, lower_bound, head_gain, recur_state,
    w_out, mixer_gain, w_up, w_down,
):
    z, x = lax.axis_index("z"), lax.axis_index("x")
    y, c = lax.axis_index("y"), lax.axis_index("core")
    t = y * NC + c
    kz = (z + jnp.arange(NZ)) % NZ
    put_at = ((kz + c) % NC * NY + (kz // NC - y) % NY).astype(jnp.int32)
    x_at = ((x + jnp.arange(NX)) % NX).astype(jnp.int32)
    z_at = z.reshape(1).astype(jnp.int32)
    k_at = ((t - z) % NZ).reshape(1).astype(jnp.int32)

    tok = exchange(call(spread_kernel, shape(NX * NT, 8, 128), tokens), XTP)
    moved = swap_rows(tokens)
    w_in = call(
        fold_kernel, local(64, 1024), w_query, w_forget, w_input, w_gate, norm_gain.reshape(64, 1)
    )
    w_ins = [w_in] + [to_x(w_in, -k) for k in range(1, NX)]

    out_t = w_out.T.reshape(4, 16, 256)
    out_t = jnp.concatenate([out_t[j] for j in range(4)], axis=1)
    w_up = (w_up.astype(F32) * mixer_gain[:, None]).astype(BF)
    bundle = jnp.concatenate([w_up, w_down.T, out_t], axis=0)
    shards = [bundle] + [None] * (NZ - 1)
    far = to_z(out_t, 4)
    up, down = bundle, bundle
    for k in (1, 2):
        up, down = to_z(up, 1), to_z(down, -1)
        shards[NZ - k], shards[k] = up, down

    parts = call(
        project_kernel, shape(NZ, 16, 1024), x_at, tok, *w_ins,
        scratch=[pltpu.VMEM((NX, 128, 64), BF)],
    )
    msg = exchange(parts, "z")
    mixture, next_state = pl.pallas_call(
        recur_kernel,
        out_shape=[local(16, 256), shape(12, 2, 128, 128, dtype=F32)],
        in_specs=[pl.BlockSpec(memory_space=pltpu.SMEM)]
        + [pl.BlockSpec(memory_space=pltpu.VMEM)] * 3
        + [pl.BlockSpec(memory_space=pl.ANY)],
        out_specs=[pl.BlockSpec(memory_space=pltpu.VMEM), pl.BlockSpec(memory_space=pl.ANY)],
        scratch_shapes=[
            pltpu.VMEM((12, 2, 128, 128), F32),
            pltpu.VMEM((12, 2, 128, 128), F32),
            pltpu.SemaphoreType.DMA((12,)),
            pltpu.SemaphoreType.DMA((12,)),
        ],
    )(
        z_at,
        pltpu.with_memory_space_constraint(msg, pltpu.VMEM),
        lower_bound.reshape(1, 256),
        head_gain,
        recur_state,
    )
    up, down = to_z(after(up, msg), 1), to_z(after(down, mixture), -1)
    shards[5], shards[3] = up, down

    mixes = [mixture] + [to_x(mixture, -k) for k in (2, 1, 3)]
    mixes = [mixes[0], mixes[2], mixes[1], mixes[3]]
    block = lax.broadcasted_iota(jnp.int32, (48, 512), 1) // 64
    spread = jnp.where(block == k_at[0], jnp.tile(moved, (1, NZ)), jnp.zeros((), BF))
    attn = call(
        attend_kernel, local(48, 512), x_at, *mixes, *shards[:4], far, *shards[5:], spread,
        scratch=[pltpu.VMEM((NX, 16, 256), BF)],
    )
    pair = to_core(attn)
    fourth_up = to_z(after(up[:64], attn), 1)
    fourth_down = to_z(after(down[64:128], attn), -1)
    duo = call(pair_kernel, local(48, 512), attn, pair)
    sums = [duo] + [to_y(duo, k) for k in (2, 1, 3)]
    mixed, wide = call(
        up_kernel, [local(48, 512), local(48, 1152)], *sums, *shards[:4], fourth_up, *shards[5:]
    )
    wides = [wide] + [to_x(wide, k) for k in (2, 1, 3)]
    keep, give = call(
        down_kernel, [local(NY, 48, 64)] * 2, put_at, *wides, *shards[:4], fourth_down, *shards[5:],
        scratch=[pltpu.VMEM((NZ, 48, 64), BF)],
    )
    lasts = call(halve_kernel, [local(48, 64)] * NY, keep, to_core(give))
    lasts = [lasts[0]] + [to_y(lasts[k], k) for k in (2, 1, 3)]
    rows = call(
        last_kernel, local(48, 64), k_at, mixed, *lasts,
        scratch=[pltpu.VMEM((NZ, 48, 64), BF)],
    )
    return (swap_rows(rows), next_state)


def solution(mesh):
    devices = mesh.devices.reshape(NZ, NX, NY, NC)
    kv, tp = ("z", "x"), TP
    in_specs = (
        P(tp, kv),
        P(kv),
        P(kv, tp),
        P(kv, tp),
        P(kv, tp),
        P(kv, tp),
        P(tp),
        P(tp, None),
        P(kv, tp, None, None),
        P(tp, kv),
        P(kv),
        P(kv, tp),
        P(tp, kv),
    )
    out_specs = (P(tp, kv), P(kv, tp, None, None))
    return jax.shard_map(
        body, mesh=Mesh(devices, AXES), in_specs=in_specs, out_specs=out_specs, check_vma=False
    )
```
